32 devices in a mesh: rep: 2 (over x), fs: 8 (over z, y), tp: 2 (over core).
Axes of the slice: x: 2, y: 2, z: 4, core: 2. Of those that a mesh axis runs over, the one named last changes fastest.
Arguments:
- inputs: bfloat16 [2, 3072, 2048], P('rep', 'fs', 'tp'), may hold values from -6 to 6
- gate_proj: bfloat16 [2048, 2816], P('fs', 'tp'), may hold values from -0.125 to 0.125
- value_proj: bfloat16 [2048, 2816], P('fs', 'tp'), may hold values from -0.125 to 0.125
- gate_taps: float32 [3, 2816], replicated, may hold values from -3 to 3
- value_taps: float32 [3, 2816], replicated, may hold values from -3 to 3
- out_grad: bfloat16 [2, 3072, 2816], P('rep', 'fs', 'tp'), may hold values from -6 to 6
Outputs:
- in_grad: bfloat16 [2, 3072, 2048], P('rep', 'fs', 'tp')
- gate_proj_grad: float32 [2048, 2816], P('fs', 'tp')
- value_proj_grad: float32 [2048, 2816], P('fs', 'tp')
- gate_taps_grad: float32 [3, 2816], replicated
- value_taps_grad: float32 [3, 2816], replicated
The draws below stay inside these ranges and needn't reach their ends.
All inputs are finite; a program needn't handle non-finite values.
Results may differ from the reference program's by a relative error of at most 0.013.
Values may be sent and summed in bfloat16 or wider, within the bound.
No kernel may reach another device: no remote copies, remote signals or barrier semaphores. Data moves between devices by JAX's collectives and lax.ppermute only.
A program may use at most 128 MiB of HBM per device.

```python
import jax
import jax.numpy as jnp
from jax import lax

D = 2048
FF = 2816
CONV = 3
HID_DEV = 1408
BATCH = 2
SEQ = 3072
ALL_TOKENS = 6144


def raised(drawn, rng, source, target, shards_of, factor):
    owner, partner = [(jnp.arange(drawn.shape[axis_at]) // (drawn.shape[axis_at] // shards_of)).reshape([-1 if axis == axis_at else 1 for axis in range(drawn.ndim)]) for axis_at in (source, target)]
    chosen = jax.random.permutation(rng, shards_of)[partner]
    strong = (owner == chosen) | (owner == (partner + shards_of // 2) % shards_of)
    return jnp.where(strong, factor * drawn, drawn)


def block_scale(stream_key, extent, shards, least, largest):
    def one(position, blocks):
        draws = jax.random.uniform(jax.random.fold_in(jax.random.fold_in(stream_key, 6), position), (blocks,), jnp.float32, least / len(shards), largest / len(shards))
        return jnp.repeat(jnp.exp(draws), extent[position] // blocks).reshape((-1,) + (1,) * (len(extent) - position - 1))

    factor_of = one(*shards[0])
    for cut in shards[1:]:
        factor_of = factor_of * one(*cut)
    return factor_of


def centred(stream_key, extent, deviation, limit, split=(), kind=jnp.bfloat16):
    level = block_scale(stream_key, extent, split, -0.22, 0.18) if split else 1.0
    result = jax.random.normal(stream_key, extent, jnp.float32) * deviation * level
    return jnp.minimum(jnp.maximum(result, -limit), limit).astype(kind)


def bell_draw_with(key, dims, deviation, bound, split, heavy, kind=jnp.bfloat16):
    array = deviation * jax.random.normal(key, dims, jnp.float32)
    if split:
        array = array * block_scale(key, dims, split, -0.22, 0.18)
    return jnp.clip(raised(array, jax.random.fold_in(key, 3), *heavy), -bound, bound).astype(kind)


def setup_inputs(seed: int = 0) -> dict:
    arg_keys = jax.random.split(jax.random.key(seed), 7)
    inputs = bell_draw_with(arg_keys[0], (BATCH, SEQ, D), 1.0, 6.0, ((0, 2), (1, 8), (2, 2)), (1, 2, 8, 2.0))
    gate_proj = centred(arg_keys[1], (D, FF), D ** -0.5, 0.125, ((0, 8), (1, 2)))
    value_proj = centred(arg_keys[2], (D, FF), D ** -0.5, 0.125, ((0, 8), (1, 2)))
    gate_taps = centred(arg_keys[3], (CONV, FF), 0.577, 3.0, (), jnp.float32)
    value_taps = centred(arg_keys[4], (CONV, FF), 0.577, 3.0, (), jnp.float32)
    out_grad = bell_draw_with(arg_keys[5], (BATCH, SEQ, FF), 1.0, 6.0, ((0, 2), (1, 8), (2, 2)), (1, 2, 8, 2.0))
    return dict(inputs=inputs, gate_proj=gate_proj, value_proj=value_proj, gate_taps=gate_taps, value_taps=value_taps, out_grad=out_grad)


def conv_fwd(pre_acts, taps):
    seq_len = pre_acts.shape[0]
    padded = jnp.pad(pre_acts, ((1, 1), (0, 0)))
    return taps[0] * padded[0:seq_len] + taps[1] * padded[1:seq_len + 1] + taps[2] * padded[2:seq_len + 2]


def conv_back(cot_rows, taps):
    seq_len = cot_rows.shape[0]
    padded = jnp.pad(cot_rows, ((1, 1), (0, 0)))
    return taps[0] * padded[2:seq_len + 2] + taps[1] * padded[1:seq_len + 1] + taps[2] * padded[0:seq_len]


def cotangents(gate_mix, value_mix, cot_in):
    sigmoid_gate = jax.nn.sigmoid(gate_mix)
    gate_cot = cot_in * value_mix * (sigmoid_gate * (1.0 + gate_mix * (1.0 - sigmoid_gate)))
    value_cot = cot_in * (gate_mix * sigmoid_gate)
    return gate_cot, value_cot


def reference(inputs, gate_proj, value_proj, gate_taps, value_taps, out_grad):
    contract_cols = (((1,), (1,)), ((), ()))
    contract_rows = (((0,), (0,)), ((), ()))

    def one_sequence(pair):
        seq_inputs, seq_cot = pair
        seq_len = seq_inputs.shape[0]
        gate_pre = jnp.dot(seq_inputs, gate_proj, preferred_element_type=jnp.float32).astype(jnp.bfloat16)
        value_pre = jnp.dot(seq_inputs, value_proj, preferred_element_type=jnp.float32).astype(jnp.bfloat16)
        gate_mix = conv_fwd(gate_pre.astype(jnp.float32), gate_taps)
        value_mix = conv_fwd(value_pre.astype(jnp.float32), value_taps)
        gate_cot, value_cot = cotangents(gate_mix, value_mix, seq_cot.astype(jnp.float32))
        gate_pre_cot = conv_back(gate_cot, gate_taps).astype(jnp.bfloat16)
        value_pre_cot = conv_back(value_cot, value_taps).astype(jnp.bfloat16)

        def add_block(total, block_index):
            first_col = (block_index * HID_DEV).astype(jnp.int32)
            gate_cols = lax.dynamic_slice_in_dim(gate_pre_cot, first_col, HID_DEV, 1)
            value_cols = lax.dynamic_slice_in_dim(value_pre_cot, first_col, HID_DEV, 1)
            gate_block = lax.dynamic_slice_in_dim(gate_proj, first_col, HID_DEV, 1)
            value_block = lax.dynamic_slice_in_dim(value_proj, first_col, HID_DEV, 1)
            partial_value = lax.dot_general(gate_cols, gate_block, contract_cols, preferred_element_type=jnp.float32)
            partial_value = partial_value + lax.dot_general(value_cols, value_block, contract_cols, preferred_element_type=jnp.float32)
            rounded = lax.optimization_barrier(partial_value.astype(jnp.bfloat16))
            return total + rounded.astype(jnp.float32), None

        in_sum, _ = lax.scan(add_block, jnp.zeros((seq_len, D), jnp.float32), jnp.arange(FF // HID_DEV).astype(jnp.int32))
        in_grad = in_sum.astype(jnp.bfloat16)
        gate_grad = lax.dot_general(seq_inputs, gate_pre_cot, contract_rows, preferred_element_type=jnp.float32)
        value_grad = lax.dot_general(seq_inputs, value_pre_cot, contract_rows, preferred_element_type=jnp.float32)
        gate_padded = jnp.pad(gate_pre.astype(jnp.float32), ((1, 1), (0, 0)))
        value_padded = jnp.pad(value_pre.astype(jnp.float32), ((1, 1), (0, 0)))
        gate_tgrad = jnp.stack([jnp.sum(gate_padded[offset:offset + seq_len] * gate_cot, axis=0) for offset in range(3)])
        value_tgrad = jnp.stack([jnp.sum(value_padded[offset:offset + seq_len] * value_cot, axis=0) for offset in range(3)])
        return in_grad, gate_grad, value_grad, gate_tgrad, value_tgrad

    results = lax.map(one_sequence, (inputs, out_grad))
    factor = float(ALL_TOKENS) ** -0.5
    return (results[0], jnp.sum(results[1], axis=0) * factor, jnp.sum(results[2], axis=0) * factor,
            jnp.sum(results[3], axis=0) * factor, jnp.sum(results[4], axis=0) * factor)
```

```python
import functools

import jax
import jax.numpy as jnp
from jax import lax
from jax.experimental import pallas as pl
from jax.experimental.pallas import tpu as pltpu
from jax.sharding import PartitionSpec as P

BF16 = jnp.bfloat16
F32 = jnp.float32
TAIL = 8
NT = (((1,), (1,)), ((), ()))
NN = (((1,), (0,)), ((), ()))


def front_kernel(dims, ids, taps, *refs):
    toks, feats, part, padp, width, planes, cores, count, n_src, src_cols, factor = dims
    it = iter(refs)
    w_refs = [(next(it), next(it)) for _ in range(n_src)]
    x_refs = [[next(it) for _ in range(cores)] for _ in range(count)]
    c_refs = [next(it) for _ in range(count)]
    pc_out, w_out, taps_out = next(it), next(it), next(it)
    g_out = [next(it) for _ in range(planes)]
    xbuf, wbuf, cbuf, pre, pct, gbuf, pcbuf, w_sem, x_sem, c_sem, o_sem = it
    plane, core = ids[0], ids[1]
    main = count * toks

    copies_w = []
    for i, (first, second) in enumerate(w_refs):
        col = pl.multiple_of(ids[2 + 2 * i], 128)
        flag = ids[3 + 2 * i]
        for b in range(2):
            def make(src, b=b, i=i, col=col):
                return pltpu.make_async_copy(
                    src.at[pl.ds(b * part, part)],
                    wbuf.at[pl.ds(b * padp, part), pl.ds(col, src_cols)],
                    w_sem.at[2 * i + b],
                )
            pl.when(flag == 0)(lambda make=make, first=first: make(first).start())
            pl.when(flag != 0)(lambda make=make, second=second: make(second).start())
            copies_w.append(make(first))
    copies_x = []
    for j in range(count):
        for k in range(cores):
            col = pl.multiple_of(lax.rem(core - k + cores, cores) * feats, 128)
            src = x_refs[j][k]
            a = pltpu.make_async_copy(
                src.at[pl.ds(0, toks)],
                xbuf.at[pl.ds(j * toks, toks), pl.ds(col, feats)],
                x_sem.at[0, j * cores + k],
            )
            b = pltpu.make_async_copy(
                src.at[pl.ds(toks, TAIL)],
                xbuf.at[pl.ds(main + j * TAIL, TAIL), pl.ds(col, feats)],
                x_sem.at[1, j * cores + k],
            )
            a.start()
            b.start()
            copies_x += [a, b]
    copies_c = []
    for j in range(count):
        c = pltpu.make_async_copy(c_refs[j], cbuf.at[j], c_sem.at[j])
        c.start()
        copies_c.append(c)
    if padp > part:
        zeros = jnp.zeros((padp - part, width), BF16)
        wbuf[part:padp, :] = zeros
        wbuf[padp + part :, :] = zeros
    taps_out[...] = jnp.zeros_like(taps_out)
    for c in copies_w + copies_x + copies_c:
        c.wait()
    w_copy = pltpu.make_async_copy(wbuf, w_out, o_sem.at[0])
    w_copy.start()

    tails = lax.dot_general(
        xbuf[main:, :], wbuf[...], NT, preferred_element_type=F32
    )
    pre[:, toks:, :] = tails.reshape(count, TAIL, 2 * padp)

    def one_block(j, carry):
        at = pl.multiple_of(j * toks, toks)
        pre[j, 0:toks, :] = lax.dot_general(
            xbuf[pl.ds(at, toks), :], wbuf[...], NT, preferred_element_type=F32
        )
        ext = toks + TAIL
        for s in range(padp // 128):
            gl = slice(s * 128, s * 128 + 128)
            vl = slice(padp + s * 128, padp + s * 128 + 128)

            def parts(lanes):
                v = pre[j, :, lanes].astype(BF16).astype(F32)
                return pltpu.roll(v, 1, 0), v, pltpu.roll(v, ext - 1, 0)

            gp, vp = parts(gl), parts(vl)
            gt = [taps[o : o + 1, gl] for o in range(3)]
            vt = [taps[o : o + 1, vl] for o in range(3)]
            gate_mix = gt[0] * gp[0] + gt[1] * gp[1] + gt[2] * gp[2]
            value_mix = vt[0] * vp[0] + vt[1] * vp[1] + vt[2] * vp[2]
            cot = cbuf[j, :, gl].astype(F32)
            sig = jax.nn.sigmoid(gate_mix)
            gate_cot = cot * value_mix * (sig * (1.0 + gate_mix * (1.0 - sig)))
            value_cot = cot * (gate_mix * sig)
            for lanes, p, t, c in ((gl, gp, gt, gate_cot), (vl, vp, vt, value_cot)):
                for o in range(3):
                    taps_out[o : o + 1, lanes] += jnp.sum(
                        p[o][0:toks] * c[0:toks], axis=0, keepdims=True
                    )
                back = t[0] * pltpu.roll(c, ext - 1, 0) + t[1] * c + t[2] * pltpu.roll(c, 1, 0)
                back = back[0:toks]
                pcbuf[pl.ds(at, toks), lanes] = back.astype(BF16)
                pct[lanes, pl.ds(at, toks)] = back.T.astype(BF16)
        return carry

    lax.fori_loop(0, count, one_block, 0)
    pc_copy = pltpu.make_async_copy(pcbuf, pc_out, o_sem.at[1])
    pc_copy.start()
    block = width // planes
    done = []
    for m in range(planes):
        col = pl.multiple_of(lax.rem(plane + m, planes) * block, 128)
        g = lax.dot_general(
            pct[...], xbuf[0:main, pl.ds(col, block)], NN, preferred_element_type=F32
        )
        g = (g * factor).astype(BF16)
        gbuf[m, 0:part, :] = g[0:part]
        gbuf[m, part:, :] = g[padp : padp + part]
        c = pltpu.make_async_copy(gbuf.at[m], g_out[m], o_sem.at[2 + m])
        c.start()
        done.append(c)
    for c in [w_copy, pc_copy] + done:
        c.wait()


def back_kernel(dims, ids, pc, w, *refs):
    toks, feats, cores, count = dims
    outs, (buf, sem) = refs[: cores * count], refs[cores * count :]
    core = ids[1]
    copies = []
    for j in range(count):
        for k in range(cores):
            i = j * cores + k
            col = pl.multiple_of(lax.rem(core + k, cores) * feats, 128)
            buf[i] = lax.dot_general(
                pc[j * toks : (j + 1) * toks, :],
                w[:, pl.ds(col, feats)],
                NN,
                preferred_element_type=F32,
            ).astype(BF16)
            c = pltpu.make_async_copy(buf.at[i], outs[i], sem.at[i])
            c.start()
            copies.append(c)
    for c in copies:
        c.wait()


def shards(inputs, gate_proj, value_proj, gate_taps, value_taps, out_grad):
    reps, fs_count, cores = (lax.axis_size(a) for a in ("rep", "fs", "tp"))
    cols = 2 if fs_count % 2 == 0 else 1
    planes = fs_count // cols
    fs_at = lax.axis_index("fs")
    rep_at, plane_at, col_at, core_at = (
        lax.axis_index("rep"),
        fs_at // cols,
        fs_at % cols,
        lax.axis_index("tp"),
    )
    group = reps * cols
    toks, feats = inputs.shape[1:]
    rows, hid = gate_proj.shape
    part = hid // group
    padp = -(-part // 128) * 128
    width = feats * cores
    factor = float(toks * fs_count * reps) ** (-0.5)

    def member(dr, dc):
        return ((rep_at + dr) % reps) * cols + (col_at + dc) % cols

    def to_member(value, dr, dc):
        perm = []
        for r in range(reps):
            for f in range(fs_count):
                p, k = f // cols, f % cols
                to = ((r + dr) % reps) * fs_count + p * cols + (k + dc) % cols
                perm.append((r * fs_count + f, to))
        return lax.ppermute(value, ("rep", "fs"), perm)

    def to_plane(value, step, first, last):
        perm = [
            (p * cols + k, (p + step) * cols + k)
            for p in range(first, last)
            for k in range(cols)
            if 0 <= p + step < planes
        ]
        return lax.ppermute(value, "fs", perm)

    def ring_plane(value, step):
        perm = [
            (p * cols + k, ((p + step) % planes) * cols + k)
            for p in range(planes)
            for k in range(cols)
        ]
        return lax.ppermute(value, "fs", perm)

    def next_pos(value, step):
        perm = [(f, f + step) for f in range(fs_count) if 0 <= f + step < fs_count]
        return lax.ppermute(value, "fs", perm)

    def core_shift(value, k):
        return lax.ppermute(value, "tp", [(i, (i + k) % cores) for i in range(cores)])

    offsets = [(dr, dc) for dr in range(reps) for dc in range(cols)]
    count = len(offsets)

    slabs = jnp.concatenate(
        [
            gate_proj.T.reshape(group, part, rows),
            value_proj.T.reshape(group, part, rows),
        ],
        axis=1,
    )
    sources, ids = [], [plane_at, core_at]
    for dc in range(cols):
        piece = lax.dynamic_index_in_dim(slabs, member(0, dc), 0, keepdims=False)
        if dc:
            piece = to_member(piece, 0, dc)
        k = (col_at - dc) % cols
        ups, downs = {}, {}
        up = down = piece
        for step in range(1, planes):
            up = ups[step] = to_plane(up, 1, step - 1, planes)
            down = downs[step] = to_plane(down, -1, 0, planes - step + 1)
        sources.append((piece, piece))
        ids += [(plane_at * cols + k) * rows, 0]
        for step in range(1, planes):
            sources.append((ups[step], downs[planes - step]))
            ids += [
                ((plane_at - step) % planes * cols + k) * rows,
                (plane_at < step).astype(jnp.int32),
            ]
    src_cols = rows
    if rows % 128:
        pieces = jnp.stack(
            [jnp.where(ids[3 + 2 * i] == 0, a, b) for i, (a, b) in enumerate(sources)]
        )
        order = jnp.argsort(jnp.stack([ids[2 + 2 * i] for i in range(len(sources))]))
        whole = pieces[order].transpose(1, 0, 2).reshape(2 * part, width)
        sources, ids, src_cols = [(whole, whole)], [plane_at, core_at, 0, 0], width
    ids = jnp.stack([jnp.asarray(i, jnp.int32) for i in ids])

    own, cot = inputs[0], out_grad[0]
    gap = jnp.zeros((TAIL - 4, feats), BF16)
    block = jnp.concatenate(
        [own, next_pos(own[:2], -1), gap, next_pos(own[toks - 2 :], 1)], axis=0
    )
    gap = jnp.zeros((TAIL - 2, hid), BF16)
    cot = jnp.concatenate([cot, next_pos(cot[:1], -1), gap, next_pos(cot[toks - 1 :], 1)], axis=0)
    cot = jnp.pad(cot, ((0, 0), (0, padp - part)))
    x_blocks, c_blocks = [], []
    for dr, dc in offsets:
        cot_part = lax.dynamic_slice_in_dim(cot, member(dr, dc) * part, padp, 1)
        mine = block
        if (dr, dc) != (0, 0):
            mine = to_member(block, dr, dc)
            cot_part = to_member(cot_part, dr, dc)
        x_blocks.append([mine] + [core_shift(mine, k) for k in range(1, cores)])
        c_blocks.append(cot_part)

    first_col = core_at * hid + member(0, 0) * part
    taps = jnp.concatenate(
        [
            jnp.pad(
                lax.dynamic_slice_in_dim(t, first_col, part, 1), ((0, 5), (0, padp - part))
            )
            for t in (gate_taps, value_taps)
        ],
        axis=1,
    )

    anywhere = pl.BlockSpec(memory_space=pl.ANY)
    vmem = pl.BlockSpec(memory_space=pltpu.VMEM)
    smem = pl.BlockSpec(memory_space=pltpu.SMEM)
    main = count * toks
    block_cols = width // planes
    n_src = len(sources)
    dims = (toks, feats, part, padp, width, planes, cores, count, n_src, src_cols, factor)
    operands = [a for pair in sources for a in pair]
    operands += [a for row in x_blocks for a in row] + c_blocks
    flops = 2 * 2 * main * 2 * padp * width
    outs = pl.pallas_call(
        functools.partial(front_kernel, dims),
        out_shape=[
            jax.ShapeDtypeStruct((main, 2 * padp), BF16),
            jax.ShapeDtypeStruct((2 * padp, width), BF16),
            jax.ShapeDtypeStruct((8, 2 * padp), F32),
        ]
        + [jax.ShapeDtypeStruct((2 * part, block_cols), BF16)] * planes,
        in_specs=[smem, vmem] + [anywhere] * len(operands),
        out_specs=[anywhere, anywhere, vmem] + [anywhere] * planes,
        scratch_shapes=[
            pltpu.VMEM((main + count * TAIL, width), BF16),
            pltpu.VMEM((2 * padp, width), BF16),
            pltpu.VMEM((count, toks + TAIL, padp), BF16),
            pltpu.VMEM((count, toks + TAIL, 2 * padp), F32),
            pltpu.VMEM((2 * padp, main), BF16),
            pltpu.VMEM((planes, 2 * part, block_cols), BF16),
            pltpu.VMEM((main, 2 * padp), BF16),
            pltpu.SemaphoreType.DMA((2 * n_src,)),
            pltpu.SemaphoreType.DMA((2, count * cores)),
            pltpu.SemaphoreType.DMA((count,)),
            pltpu.SemaphoreType.DMA((2 + planes,)),
        ],
        compiler_params=pltpu.CompilerParams(vmem_limit_bytes=60 * 1024 * 1024),
        cost_estimate=pl.CostEstimate(
            flops=flops, bytes_accessed=24 * 1024 * 1024, transcendentals=main * padp
        ),
        name="front",
    )(ids, taps, *operands)
    pre_cot, weight, tap_terms = outs[:3]
    grads = outs[3:]

    up = down = None
    for step in range(1, planes):
        to_up, to_down = grads[planes - step], grads[step]
        if up is not None:
            to_up = (to_up.astype(F32) + up.astype(F32)).astype(BF16)
            to_down = (to_down.astype(F32) + down.astype(F32)).astype(BF16)
        up = to_plane(to_up, 1, 0, step)
        down = to_plane(to_down, -1, planes - step, planes)
    total = grads[0]
    if up is not None:
        total = (total.astype(F32) + up.astype(F32) + down.astype(F32)).astype(BF16)
    total = total.reshape(2 * part, cols, rows)
    gathered = jnp.zeros((group, 2 * part, rows), BF16)
    for dr, dc in offsets:
        piece = lax.dynamic_index_in_dim(total, (col_at + dc) % cols, 1, keepdims=False)
        if (dr, dc) != (0, 0):
            piece = to_member(piece, dr, dc)
        gathered = lax.dynamic_update_slice(gathered, piece[None], (member(-dr, -dc), 0, 0))
    gathered = gathered.reshape(group, 2, part, rows)
    gate_grad = gathered[:, 0].reshape(hid, rows).T.astype(F32)
    value_grad = gathered[:, 1].reshape(hid, rows).T.astype(F32)

    partials = pl.pallas_call(
        functools.partial(back_kernel, (toks, feats, cores, count)),
        out_shape=[jax.ShapeDtypeStruct((toks, feats), BF16)] * (cores * count),
        in_specs=[smem, vmem, vmem],
        out_specs=[anywhere] * (cores * count),
        scratch_shapes=[
            pltpu.VMEM((cores * count, toks, feats), BF16),
            pltpu.SemaphoreType.DMA((cores * count,)),
        ],
        compiler_params=pltpu.CompilerParams(vmem_limit_bytes=40 * 1024 * 1024),
        cost_estimate=pl.CostEstimate(
            flops=flops // 2, bytes_accessed=12 * 1024 * 1024, transcendentals=0
        ),
        name="back",
    )(ids, pre_cot, weight)
    in_sum = None
    for j, (dr, dc) in enumerate(offsets):
        mine = partials[j * cores].astype(F32)
        for k in range(1, cores):
            mine = mine + core_shift(partials[j * cores + k], k).astype(F32)
        if (dr, dc) != (0, 0):
            mine = to_member(mine.astype(BF16), -dr, -dc).astype(F32)
        in_sum = mine if in_sum is None else in_sum + mine
    in_grad = in_sum.astype(BF16)[None]

    tap_sum = tap_terms
    for step in range(1, planes):
        tap_sum = tap_sum + ring_plane(tap_terms, step)
    tap_sum = tap_sum * factor
    mine = jnp.zeros((group, 8, 2 * padp), F32)
    for dr, dc in offsets:
        got = tap_sum if (dr, dc) == (0, 0) else to_member(tap_sum, dr, dc)
        mine = lax.dynamic_update_slice(mine, got[None], (member(-dr, -dc), 0, 0))
    mine = mine[:, :3].reshape(group, 3, 2, padp)[..., :part]
    mine = mine.transpose(2, 1, 0, 3).reshape(2, 3, hid)
    taps_all = jnp.zeros((2, 3, cores * hid), F32)
    for k in range(cores):
        got = mine if k == 0 else core_shift(mine, k)
        taps_all = lax.dynamic_update_slice(taps_all, got, (0, 0, (core_at - k) % cores * hid))
    return in_grad, gate_grad, value_grad, taps_all[0], taps_all[1]


def solution(mesh):
    placed = (P("rep", "fs", "tp"), P("fs", "tp"), P("fs", "tp"), P(), P(), P("rep", "fs", "tp"))
    return jax.shard_map(
        shards,
        mesh=mesh,
        in_specs=placed,
        out_specs=(P("rep", "fs", "tp"), P("fs", "tp"), P("fs", "tp"), P(), P()),
        check_vma=False,
    )
```
